256 devices in a mesh: sp: 16 (over y, x), tp: 16 (over z, core).
Axes of the slice: x: 4, y: 4, z: 8, core: 2. Of those that a mesh axis runs over, the one named last changes fastest.
Arguments:
- residual: bfloat16 [16384, 2048], P(('sp', 'tp')), may hold values from -6 to 6
- wide_query: bfloat16 [16384, 1024], P('sp', 'tp'), may hold values from -8 to 8
- narrow_query: bfloat16 [16384, 1024], P('sp', 'tp'), may hold values from -8 to 8
- wide_keys: bfloat16 [16384, 256], P('sp'), may hold values from -6 to 6
- narrow_keys: bfloat16 [16384, 256], P('sp'), may hold values from -6 to 6
- wide_values: bfloat16 [16384, 256], P('sp'), may hold values from -6 to 6
- narrow_values: bfloat16 [16384, 256], P('sp'), may hold values from -6 to 6
- wide_query_gain: float32 [64], replicated, may hold values from 1.2 to 10
- wide_key_gain: float32 [64], replicated, may hold values from 1.2 to 10
- narrow_query_gain: float32 [32], replicated, may hold values from 1.2 to 10
- narrow_key_gain: float32 [32], replicated, may hold values from 1.2 to 10
- wide_out: bfloat16 [1024, 2048], P('tp'), may hold values from -0.25 to 0.25
- narrow_out: bfloat16 [1024, 2048], P('tp'), may hold values from -0.25 to 0.25
- first_gain: float32 [2048], replicated, may hold values from 0.1 to 1.9
- first_bias: float32 [2048], replicated, may hold values from -1.8 to 1.8
- route_ids: int32 [16384, 2], P(('sp', 'tp')), may hold values from 0 to 31, all different within a row; in each aligned block of 64 rows (0 to 63, 64 to 127, ...) at most 5 rows name the same one
- route_weights: float32 [16384, 2], P(('sp', 'tp')), may hold values from 0.25 to 2.5
- expert_gate: bfloat16 [32, 2048, 3072], P('sp', None, 'tp'), may hold values from -0.125 to 0.125
- expert_up: bfloat16 [32, 2048, 3072], P('sp', None, 'tp'), may hold values from -0.125 to 0.125
- expert_down: bfloat16 [32, 3072, 2048], P('sp', 'tp'), may hold values from -0.109375 to 0.109375
- shared_gate: bfloat16 [2048, 256], replicated, may hold values from -0.125 to 0.125
- shared_up: bfloat16 [2048, 256], replicated, may hold values from -0.125 to 0.125
- shared_down: bfloat16 [256, 2048], replicated, may hold values from -0.375 to 0.375
- second_gain: float32 [2048], replicated, may hold values from 0.1 to 1.9
- second_bias: float32 [2048], replicated, may hold values from -1.8 to 1.8
Outputs:
- layer_output: bfloat16 [16384, 2048], P(('sp', 'tp'))
The draws below stay inside these ranges and needn't reach their ends.
Inputs may be any that keep to these rules, and one draw needn't show every extreme that they name: `route_ids`: each row names 2 different experts. The rows of one device (aligned blocks of 64 rows) name each expert at most 5 times, and in every draw some expert is named exactly 5 times in the rows of some device.
All inputs are finite; a program needn't handle non-finite values.
Results may differ from the reference program's by a relative error of at most 0.02.
The reference program's roundings to bfloat16 on the way count: a program that leaves them out, or rounds other values in their place, can miss the bound.
Values may be sent and summed in bfloat16 or wider, within the bound.
A program may use at most 128 MiB of HBM per device.

```python
import math
import jax
import jax.numpy as jnp
import numpy as np
from jax import lax

MODEL_WIDTH = 2048
WIDE_HEADS = 16
WIDE_SIZE = 64
WIDE_GROUPS = 4
NARROW_HEADS = 32
NARROW_SIZE = 32
NARROW_GROUPS = 8
GRID_WIDTH = 64
EXPERT_WIDTH = 3072
SHARED_WIDTH = 256
ROUTE_TOP = 2
SEQ_TOKENS = 4096
TOKENS = 16384
DEVICE_ROWS = 64
EXPERTS = 32
CAPACITY = 5
N_SP = 16
N_TP = 16


def gain_pair(key, head_size, salt):
    folded = jax.random.fold_in(key, salt)
    draw_one = jax.random.uniform(jax.random.fold_in(folded, 2), (head_size,), jnp.float32)
    draw_two = jax.random.uniform(jax.random.fold_in(folded, 3), (head_size,), jnp.float32)
    query_gain = 1.5 * 2.0 ** draw_one
    key_gain = 1.5 * 2.0 ** draw_two
    return (query_gain, key_gain)


def field(key, heads, head_size, salt):
    folded = jax.random.fold_in(key, salt)
    return jnp.clip(jax.random.normal(folded, (TOKENS, heads, head_size), jnp.float32), -6.0, 6.0)


def drawn_queries(key, heads, head_size, salt):
    values = field(key, heads, head_size, salt + 100)
    return values.reshape(TOKENS, heads * head_size).astype(jnp.bfloat16)


def drawn_keys(key, heads, head_size, salt):
    values = field(key, heads, head_size, salt + 300)
    return values.reshape(TOKENS, heads * head_size).astype(jnp.bfloat16)


def draw_wide_query(key, part):
    return drawn_queries(key, WIDE_HEADS, WIDE_SIZE, 11)


def draw_narrow_query(key, part):
    return drawn_queries(key, NARROW_HEADS, NARROW_SIZE, 23)


def draw_wide_keys(key, part):
    return drawn_keys(key, WIDE_GROUPS, WIDE_SIZE, 11)


def draw_narrow_keys(key, part):
    return drawn_keys(key, NARROW_GROUPS, NARROW_SIZE, 23)


def draw_wide_query_gain(key, part):
    return gain_pair(key, WIDE_SIZE, 11)[0]


def draw_wide_key_gain(key, part):
    return gain_pair(key, WIDE_SIZE, 11)[1]


def draw_narrow_query_gain(key, part):
    return gain_pair(key, NARROW_SIZE, 23)[0]


def draw_narrow_key_gain(key, part):
    return gain_pair(key, NARROW_SIZE, 23)[1]


def levels(own_key, extent, shards, smallest, top_value):
    factor_of, own = 1.0, jax.random.fold_in(own_key, 6)
    for dim, parts in shards:
        heights = jnp.exp(jax.random.uniform(jax.random.fold_in(own, dim), (parts,), jnp.float32, smallest / len(shards), top_value / len(shards)))
        factor_of = factor_of * jnp.repeat(heights, extent[dim] // parts).reshape([-1 if axis == dim else 1 for axis in range(len(extent))])
    return factor_of


def shared_out(own_key, own, number, rows, number_of, top, bound, slope):
    ranking = jax.random.permutation(own_key, number_of)
    packed, usual = shares(number_of, rows * top, bound, slope, True), shares(number_of, rows * top, bound, slope, False)
    places = jnp.arange(number_of)

    def named(sizes, rotation):
        used = int((sizes > 0).sum())
        fixed = max(1, used // 4)
        passed = fixed + (places - fixed + rotation * (used - fixed)) % max(1, number_of - fixed)
        return jnp.zeros((number_of,), jnp.int32).at[ranking[jnp.where(places < fixed, places, passed)]].set(jnp.asarray(sizes, jnp.int32))

    sizes = jnp.where(number % 4 == 0, named(packed, number // 4), named(usual, number - number // 4 - 1))
    mixed = jax.random.permutation(jax.random.fold_in(own, 3), number_of)
    giver, sink = mixed[0:number_of // 2 * 2:2], mixed[1:number_of // 2 * 2:2]
    room = jnp.minimum(sizes[giver] - 1, bound - sizes[sink]) // 2
    room = jnp.where((giver == ranking[0]) | (sink == ranking[0]) | (sizes[sink] == 0), 0, jnp.maximum(room, 0))
    passed = jax.random.randint(jax.random.fold_in(own, 4), (number_of // 2,), 0, 1 << 20) % (room + 1)
    sizes = sizes.at[giver].add(-passed).at[sink].add(passed)
    items = jnp.searchsorted(jnp.cumsum(sizes), jnp.arange(rows * top), side="right").astype(jnp.int32)
    table = items.reshape(top, rows).T
    table = table[jax.random.permutation(jax.random.fold_in(own, 1), rows)]
    rotation = jax.random.randint(jax.random.fold_in(own, 2), (rows, 1), 0, top)
    return jnp.take_along_axis(table, (jnp.arange(top)[None, :] + rotation) % top, axis=1)


def shares(number_of, total, most, lean, full):
    weights = [(1 << 20) // math.isqrt(rank ** lean) + 1 for rank in range(1, number_of + 1)]
    largest = most if full else min(most, max(-(-total // number_of), total * weights[0] // sum(weights)))
    least = 1 if total - largest >= number_of - 1 else 0
    given, surplus = [largest] + [least] * (number_of - 1), total - largest - least * (number_of - 1)
    while surplus > 0:
        movable = [i for i in range(1, number_of) if given[i] < largest] or [i for i in range(1, number_of) if given[i] < most]
        pool, left = sum([weights[i] for i in movable]), surplus
        for i in movable:
            more = min(most - given[i], max(1, left * weights[i] // pool), surplus)
            given[i] = given[i] + more
            surplus = surplus - more
    return np.array(given)


def gaussian(rng, shape, scale, limit, cuts=(), kind=jnp.bfloat16):
    values = jax.random.normal(rng, shape, jnp.float32) * scale
    if len(cuts) > 0:
        values = levels(rng, shape, cuts, -0.22, 0.18) * values
    return jnp.clip(values, min=-limit, max=limit).astype(kind)


def setup_inputs(seed: int = 0) -> dict:
    streams_of = jax.random.split(jax.random.key(seed), 26)
    residual = gaussian(streams_of[0], (TOKENS, MODEL_WIDTH), 1.0, 6.0, ((0, 256),))
    wide_query = draw_wide_query(jax.random.fold_in(streams_of[25], 71), 0)
    narrow_query = draw_narrow_query(jax.random.fold_in(streams_of[25], 71), 0)
    wide_keys = draw_wide_keys(jax.random.fold_in(streams_of[25], 71), 0)
    narrow_keys = draw_narrow_keys(jax.random.fold_in(streams_of[25], 71), 0)
    wide_values = gaussian(streams_of[5], (TOKENS, WIDE_GROUPS * WIDE_SIZE), 1.0, 6.0, ((0, 16),))
    narrow_values = gaussian(streams_of[6], (TOKENS, NARROW_GROUPS * NARROW_SIZE), 1.0, 6.0, ((0, 16),))
    wide_query_gain = draw_wide_query_gain(jax.random.fold_in(streams_of[25], 71), 0)
    wide_key_gain = draw_wide_key_gain(jax.random.fold_in(streams_of[25], 71), 0)
    narrow_query_gain = draw_narrow_query_gain(jax.random.fold_in(streams_of[25], 71), 0)
    narrow_key_gain = draw_narrow_key_gain(jax.random.fold_in(streams_of[25], 71), 0)
    wide_out = gaussian(streams_of[11], (WIDE_HEADS * WIDE_SIZE, MODEL_WIDTH), (WIDE_HEADS * WIDE_SIZE // 2) ** -0.5, 0.25, ((0, 16),))
    narrow_out = gaussian(streams_of[12], (NARROW_HEADS * NARROW_SIZE, MODEL_WIDTH), (NARROW_HEADS * NARROW_SIZE // 2) ** -0.5, 0.25, ((0, 16),))
    first_gain = jnp.clip(1.0 + 0.18 * jax.random.normal(streams_of[13], (MODEL_WIDTH,), jnp.float32), 0.1, 1.9)
    first_bias = gaussian(streams_of[14], (MODEL_WIDTH,), 0.3, 1.8, (), jnp.float32)
    route_ids_keys = jax.random.split(jax.random.fold_in(streams_of[15], 1), TOKENS // DEVICE_ROWS)
    route_ids_turns = jax.random.permutation(jax.random.fold_in(streams_of[15], 3), TOKENS // DEVICE_ROWS)
    route_ids = jax.vmap(lambda own, number: shared_out(jax.random.fold_in(streams_of[15], 2), own, number, DEVICE_ROWS, EXPERTS, ROUTE_TOP, CAPACITY, 2))(route_ids_keys, route_ids_turns).reshape((TOKENS, ROUTE_TOP))
    route_weights = jnp.clip(jnp.exp(math.log(2.5) - 2.3025851 * jax.random.uniform(streams_of[16], (TOKENS, ROUTE_TOP), jnp.float32) ** levels(streams_of[16], (TOKENS, ROUTE_TOP), ((0, 256),), -0.2, 0.2)), 0.25, 2.5)
    expert_gate = gaussian(streams_of[17], (EXPERTS, MODEL_WIDTH, EXPERT_WIDTH), MODEL_WIDTH ** -0.5, 0.125, ((0, 16), (2, 16)))
    expert_up = gaussian(streams_of[18], (EXPERTS, MODEL_WIDTH, EXPERT_WIDTH), MODEL_WIDTH ** -0.5, 0.125, ((0, 16), (2, 16)))
    expert_down = gaussian(streams_of[19], (EXPERTS, EXPERT_WIDTH, MODEL_WIDTH), EXPERT_WIDTH ** -0.5, 0.109375, ((0, 16), (1, 16)))
    shared_gate = gaussian(streams_of[20], (MODEL_WIDTH, SHARED_WIDTH), MODEL_WIDTH ** -0.5, 0.125)
    shared_up = gaussian(streams_of[21], (MODEL_WIDTH, SHARED_WIDTH), MODEL_WIDTH ** -0.5, 0.125)
    shared_down = gaussian(streams_of[22], (SHARED_WIDTH, MODEL_WIDTH), SHARED_WIDTH ** -0.5, 0.375)
    second_gain = jnp.clip(1.0 + 0.18 * jax.random.normal(streams_of[23], (MODEL_WIDTH,), jnp.float32), 0.1, 1.9)
    second_bias = gaussian(streams_of[24], (MODEL_WIDTH,), 0.3, 1.8, (), jnp.float32)
    return {"residual": residual, "wide_query": wide_query, "narrow_query": narrow_query, "wide_keys": wide_keys, "narrow_keys": narrow_keys, "wide_values": wide_values, "narrow_values": narrow_values, "wide_query_gain": wide_query_gain, "wide_key_gain": wide_key_gain, "narrow_query_gain": narrow_query_gain, "narrow_key_gain": narrow_key_gain, "wide_out": wide_out, "narrow_out": narrow_out, "first_gain": first_gain, "first_bias": first_bias, "route_ids": route_ids, "route_weights": route_weights, "expert_gate": expert_gate, "expert_up": expert_up, "expert_down": expert_down, "shared_gate": shared_gate, "shared_up": shared_up, "shared_down": shared_down, "second_gain": second_gain, "second_bias": second_bias}


EPS_HEAD = 1e-06
EPS_LAYER = 1e-05
ALPHA = 2.0 ** 0.25
THETA = 10000.0

def head_norm(values, gain_vec):
    mean_square = lax.optimization_barrier(jnp.mean(values * values, axis=-1, keepdims=True))
    return values * lax.rsqrt(mean_square + EPS_HEAD) * gain_vec

def rotate(values, position):
    half_size = values.shape[-1] // 2
    frequency = THETA ** (-jnp.arange(half_size, dtype=jnp.float32) / half_size)
    angles = position.astype(jnp.float32)[:, None] * frequency
    cosine = jnp.cos(angles)[:, None, :]
    sine_part = jnp.sin(angles)[:, None, :]
    leading = values[..., :half_size]
    trailing = values[..., half_size:]
    return jnp.concatenate([leading * cosine - trailing * sine_part, trailing * cosine + leading * sine_part], axis=-1)

def grid_rotate(values, position):
    half_size = values.shape[-1] // 2
    grid_row = position // GRID_WIDTH
    grid_col = position % GRID_WIDTH
    return jnp.concatenate([rotate(values[..., :half_size], grid_row), rotate(values[..., half_size:], grid_col)], axis=-1)

def layer_norm(values, gain_vec, bias_vec):
    center = lax.optimization_barrier(jnp.mean(values, axis=-1, keepdims=True))
    shifted = values - center
    variance = lax.optimization_barrier(jnp.mean(shifted * shifted, axis=-1, keepdims=True))
    return (shifted * lax.rsqrt(variance + EPS_LAYER) * gain_vec + bias_vec).astype(jnp.bfloat16)

def attend_group(queries, keys_all, values_all, query_gain, key_gain, heads_total, groups):
    head_size = query_gain.shape[0]
    per_group = heads_total // groups
    seq_count = TOKENS // SEQ_TOKENS
    block_rows = min(512, SEQ_TOKENS)
    position = jnp.arange(SEQ_TOKENS, dtype=jnp.int32)
    score_scale = head_size ** (-0.5)
    query_seq = queries.reshape(seq_count, SEQ_TOKENS, heads_total, head_size)
    key_seq = keys_all.reshape(seq_count, SEQ_TOKENS, groups, head_size)
    value_seq = values_all.reshape(seq_count, SEQ_TOKENS, groups, head_size)

    def one_sequence(operands):
        query_rows, key_rows, value_rows = operands
        rotated_queries = grid_rotate(head_norm(query_rows.astype(jnp.float32), query_gain), position).astype(jnp.bfloat16)
        rotated_keys = grid_rotate(head_norm(key_rows.astype(jnp.float32), key_gain), position).astype(jnp.bfloat16)
        key_float = rotated_keys.astype(jnp.float32)
        value_float = value_rows.astype(jnp.float32)
        blocks = rotated_queries.reshape(SEQ_TOKENS // block_rows, block_rows, groups, per_group, head_size)

        def one_block(query_block):
            scores = jnp.einsum('qgpd,kgd->gpqk', query_block.astype(jnp.float32), key_float) * score_scale
            largest = lax.optimization_barrier(jnp.max(scores, axis=-1, keepdims=True))
            weights = jnp.exp(scores - largest)
            weights = (weights / lax.optimization_barrier(jnp.sum(weights, axis=-1, keepdims=True))).astype(jnp.bfloat16)
            mixed_rows = jnp.einsum('gpqk,kgd->qgpd', weights.astype(jnp.float32), value_float)
            return mixed_rows.astype(jnp.bfloat16)
        mixed_all = lax.map(one_block, blocks)
        return mixed_all.reshape(SEQ_TOKENS, heads_total * head_size)
    result = lax.map(one_sequence, (query_seq, key_seq, value_seq))
    return result.reshape(TOKENS, heads_total * head_size)

def routed_sum(hidden, route_ids, route_weights, expert_gate, expert_up, expert_down):
    assignments = TOKENS * ROUTE_TOP
    most = N_SP * N_TP * CAPACITY
    flat_ids = route_ids.reshape(-1).astype(jnp.int32)
    order = jnp.argsort(flat_ids, stable=True).astype(jnp.int32)
    counts = lax.optimization_barrier(jnp.sum((flat_ids[:, None] == jnp.arange(EXPERTS, dtype=jnp.int32)[None, :]).astype(jnp.int32), axis=0))
    starts = jnp.cumsum(counts) - counts
    slot_rank = jnp.arange(most, dtype=jnp.int32)
    position_in = (starts[:, None] + slot_rank[None, :]).astype(jnp.int32)
    valid = slot_rank[None, :] < counts[:, None]
    picked = jnp.where(valid, order[jnp.minimum(position_in, assignments - 1)], assignments).astype(jnp.int32)
    token_rows = (picked // ROUTE_TOP).astype(jnp.int32)
    padded_hidden = jnp.concatenate([hidden, jnp.zeros((1, MODEL_WIDTH), jnp.bfloat16)], axis=0)
    block_width = EXPERT_WIDTH // N_TP

    def one_expert(operands):
        rows_index, gate_weight, up_weight, down_weight = operands
        rows_in = padded_hidden[rows_index]
        gate_values = jnp.dot(rows_in, gate_weight, preferred_element_type=jnp.float32)
        up_values = jnp.dot(rows_in, up_weight, preferred_element_type=jnp.float32)
        active = (jax.nn.silu(gate_values) * up_values).astype(jnp.bfloat16)
        blocks_in = active.reshape(most, N_TP, block_width).astype(jnp.float32)
        down_blocks = down_weight.reshape(N_TP, block_width, MODEL_WIDTH).astype(jnp.float32)
        partial_value = lax.optimization_barrier(jnp.einsum('mtf,tfd->tmd', blocks_in, down_blocks).astype(jnp.bfloat16))
        return lax.optimization_barrier(jnp.sum(partial_value.astype(jnp.float32), axis=0)).astype(jnp.bfloat16)
    outputs = lax.map(one_expert, (token_rows, expert_gate, expert_up, expert_down))
    padded_weights = jnp.concatenate([route_weights.reshape(-1), jnp.zeros((1,), jnp.float32)], axis=0)
    slot_weight = padded_weights[picked]
    contribution = slot_weight[:, :, None] * outputs.astype(jnp.float32)
    total = jnp.zeros((TOKENS + 1, MODEL_WIDTH), jnp.float32).at[token_rows.reshape(-1)].add(contribution.reshape(-1, MODEL_WIDTH))
    return total[:TOKENS]

def reference(residual, wide_query, narrow_query, wide_keys, narrow_keys, wide_values, narrow_values, wide_query_gain, wide_key_gain, narrow_query_gain, narrow_key_gain, wide_out, narrow_out, first_gain, first_bias, route_ids, route_weights, expert_gate, expert_up, expert_down, shared_gate, shared_up, shared_down, second_gain, second_bias):
    wide_mixed = attend_group(wide_query, wide_keys, wide_values, wide_query_gain, wide_key_gain, WIDE_HEADS, WIDE_GROUPS)
    narrow_mixed = attend_group(narrow_query, narrow_keys, narrow_values, narrow_query_gain, narrow_key_gain, NARROW_HEADS, NARROW_GROUPS)
    projected = jnp.dot(wide_mixed, wide_out, preferred_element_type=jnp.float32) + jnp.dot(narrow_mixed, narrow_out, preferred_element_type=jnp.float32)
    hidden = layer_norm(ALPHA * residual.astype(jnp.float32) + projected, first_gain, first_bias)
    routed = routed_sum(hidden, route_ids, route_weights, expert_gate, expert_up, expert_down)
    shared_gate_values = jnp.dot(hidden, shared_gate, preferred_element_type=jnp.float32)
    shared_up_values = jnp.dot(hidden, shared_up, preferred_element_type=jnp.float32)
    shared_active = (jax.nn.silu(shared_gate_values) * shared_up_values).astype(jnp.bfloat16)
    shared_output = jnp.dot(shared_active, shared_down, preferred_element_type=jnp.float32)
    return layer_norm(ALPHA * hidden.astype(jnp.float32) + routed + shared_output, second_gain, second_bias)
```

```python
import functools

import jax
import jax.numpy as jnp
import numpy as np
from jax import lax
from jax.experimental import pallas as pl
from jax.experimental.pallas import tpu as pltpu
from jax.sharding import PartitionSpec as P

WIDE_HEADS = 16
WIDE_GROUPS = 4
NARROW_HEADS = 32
NARROW_GROUPS = 8
GRID_WIDTH = 64
SEQ_SHARDS = 4
LOCAL_EXPERTS = 2


EPS_HEAD = 1e-06
EPS_LAYER = 1e-05
ALPHA = 2.0**0.25
THETA = 10000.0


def swapped(x, axis, apart):
    return lax.ppermute(x, axis, [(i, i ^ 1 << apart) for i in range(lax.axis_size(axis))])


def head_norm(values, gain_vec):
    mean_square = jnp.mean(values * values, axis=-1, keepdims=True)
    return values * lax.rsqrt(mean_square + EPS_HEAD) * gain_vec


def rotate(values, position):
    half_size = values.shape[-1] // 2
    frequency = THETA ** (-jnp.arange(half_size, dtype=jnp.float32) / half_size)
    angles = position.astype(jnp.float32)[:, None] * frequency
    cosine = jnp.cos(angles)[:, None, :]
    sine_part = jnp.sin(angles)[:, None, :]
    leading = values[..., :half_size]
    trailing = values[..., half_size:]
    return jnp.concatenate(
        [leading * cosine - trailing * sine_part, trailing * cosine + leading * sine_part], axis=-1
    )


def grid_rotate(values, position):
    half_size = values.shape[-1] // 2
    grid_row = position // GRID_WIDTH
    grid_col = position % GRID_WIDTH
    return jnp.concatenate(
        [rotate(values[..., :half_size], grid_row), rotate(values[..., half_size:], grid_col)],
        axis=-1,
    )


def layer_norm(values, gain_vec, bias_vec):
    center = jnp.mean(values, axis=-1, keepdims=True)
    shifted = values - center
    variance = jnp.mean(shifted * shifted, axis=-1, keepdims=True)
    return (shifted * lax.rsqrt(variance + EPS_LAYER) * gain_vec + bias_vec).astype(jnp.bfloat16)


def prepare(queries, key_block, value_block, query_gain, key_gain, heads_total, groups, position):
    head_size = query_gain.shape[0]
    local_heads = queries.shape[1] // head_size
    group_index = lax.axis_index("tp") * local_heads // (heads_total // groups)
    query_rows = queries.reshape(queries.shape[0], local_heads, head_size).astype(jnp.float32)
    rotated_queries = grid_rotate(head_norm(query_rows, query_gain), position).astype(jnp.bfloat16)
    column_start = group_index * head_size
    key_rows = lax.dynamic_slice_in_dim(key_block, column_start, head_size, 1).astype(jnp.float32)[
        :, None, :
    ]
    rotated_keys = grid_rotate(head_norm(key_rows, key_gain), position)[:, 0, :].astype(
        jnp.bfloat16
    )
    value_rows = lax.dynamic_slice_in_dim(value_block, column_start, head_size, 1)
    return (rotated_queries, jnp.concatenate([rotated_keys, value_rows], axis=1))


def attend_local(rotated_queries, key_block, value_block):
    seg_rows, local_heads, head_size = rotated_queries.shape
    block_rows = min(512, seg_rows)
    score_scale = head_size ** (-0.5)
    blocks = rotated_queries.reshape(seg_rows // block_rows, block_rows, local_heads, head_size)

    def one_block(query_block):
        scores = (
            jnp.einsum("qhd,kd->hqk", query_block, key_block, preferred_element_type=jnp.float32)
            * score_scale
        )
        largest = jnp.max(scores, axis=-1, keepdims=True)
        weights = jnp.exp(scores - largest)
        weights = (weights / jnp.sum(weights, axis=-1, keepdims=True)).astype(jnp.bfloat16)
        return jnp.einsum(
            "hqk,kd->qhd", weights, value_block, preferred_element_type=jnp.float32
        ).astype(jnp.bfloat16)

    mixed_rows = lax.map(one_block, blocks)
    return mixed_rows.reshape(seg_rows, local_heads * head_size)


def local(
    residual,
    wide_query,
    narrow_query,
    wide_keys,
    narrow_keys,
    wide_values,
    narrow_values,
    wide_query_gain,
    wide_key_gain,
    narrow_query_gain,
    narrow_key_gain,
    wide_out,
    narrow_out,
    first_gain,
    first_bias,
    route_ids,
    route_weights,
    expert_gate,
    expert_up,
    expert_down,
    shared_gate,
    shared_up,
    shared_down,
    second_gain,
    second_bias,
):
    seg_rows = wide_query.shape[0]
    position = lax.axis_index("sp") % SEQ_SHARDS * seg_rows + jnp.arange(seg_rows, dtype=jnp.int32)
    wide_rotated, wide_pack = prepare(
        wide_query,
        wide_keys,
        wide_values,
        wide_query_gain,
        wide_key_gain,
        WIDE_HEADS,
        WIDE_GROUPS,
        position,
    )
    narrow_rotated, narrow_pack = prepare(
        narrow_query,
        narrow_keys,
        narrow_values,
        narrow_query_gain,
        narrow_key_gain,
        NARROW_HEADS,
        NARROW_GROUPS,
        position,
    )
    gathered = jnp.concatenate([wide_pack, narrow_pack], axis=1)
    for level in range(SEQ_SHARDS.bit_length() - 1):
        partner = swapped(gathered, "sp", level)
        is_upper = lax.axis_index("sp") // 2**level % 2 == 1
        gathered = jnp.where(
            is_upper,
            jnp.concatenate([partner, gathered], axis=0),
            jnp.concatenate([gathered, partner], axis=0),
        )
    wide_size = wide_query_gain.shape[0]
    narrow_size = narrow_query_gain.shape[0]
    narrow_start = 2 * wide_size
    wide_mixed = attend_local(
        wide_rotated, gathered[:, :wide_size], gathered[:, wide_size:narrow_start]
    )
    narrow_mixed = attend_local(
        narrow_rotated,
        gathered[:, narrow_start : narrow_start + narrow_size],
        gathered[:, narrow_start + narrow_size :],
    )
    wide_tokens, narrow_tokens = (
        lax.all_to_all(wide_mixed, "tp", split_axis=0, concat_axis=1, tiled=True),
        lax.all_to_all(narrow_mixed, "tp", split_axis=0, concat_axis=1, tiled=True),
    )
    running = jnp.dot(
        wide_tokens,
        lax.all_gather(wide_out, "tp", axis=0, tiled=True),
        preferred_element_type=jnp.float32,
    )
    projected = running + jnp.dot(
        narrow_tokens,
        lax.all_gather(narrow_out, "tp", axis=0, tiled=True),
        preferred_element_type=jnp.float32,
    )
    hidden = layer_norm(ALPHA * residual.astype(jnp.float32) + projected, first_gain, first_bias)
    device_rows = hidden.shape[0]
    sp_size = lax.axis_size("sp")
    top_count = route_ids.shape[1]
    experts = LOCAL_EXPERTS * sp_size
    flat_ids = route_ids.reshape(-1)
    expert_hits = (flat_ids[:, None] == jnp.arange(experts, dtype=jnp.int32)[None, :]).astype(
        jnp.int32
    )
    earlier = jnp.sum((jnp.cumsum(expert_hits, axis=0) - expert_hits) * expert_hits, axis=1)
    slot_index = flat_ids * SLOT + earlier
    chosen = (
        slot_index[:, None] == jnp.arange(experts * SLOT, dtype=jnp.int32)[None, :]
    ).astype(jnp.float32)
    chosen = chosen.reshape(device_rows, top_count, experts * SLOT)
    placing = jnp.sum(chosen, axis=1).astype(jnp.bfloat16)
    mixing = jnp.sum(chosen * route_weights[:, :, None], axis=1)
    outgoing = jnp.einsum("rs,rd->sd", placing, hidden, preferred_element_type=jnp.float32).astype(
        jnp.bfloat16
    )
    routed = moe(
        outgoing,
        mixing,
        expert_gate,
        expert_up,
        expert_down,
        sp_size,
        lax.axis_size("tp") // 2,
    )
    shared_gate_values = jnp.dot(hidden, shared_gate, preferred_element_type=jnp.float32)
    shared_up_values = jnp.dot(hidden, shared_up, preferred_element_type=jnp.float32)
    shared_active = (jax.nn.silu(shared_gate_values) * shared_up_values).astype(jnp.bfloat16)
    shared_output = jnp.dot(shared_active, shared_down, preferred_element_type=jnp.float32)
    return layer_norm(
        ALPHA * hidden.astype(jnp.float32) + routed + shared_output, second_gain, second_bias
    )


CAPACITY = 5
SLOT = 8
MESH = pl.DeviceIdType.MESH


def moe_kernel(
    n_sp,
    n_z,
    outgoing,
    mixing,
    pack,
    spread,
    gate_hbm,
    up_hbm,
    down_hbm,
    routed,
    arrived,
    blocks,
    sums,
    landing,
    sending,
    returned,
    gate_w,
    up_w,
    down_w,
    hand_send,
    hand_recv,
    ring_send,
    ring_recv,
    sum_send,
    sum_recv,
    back_send,
    back_recv,
    own_sem,
    pair_send,
    pair_recv,
):
    half = n_z // 2
    peers = 2 * n_sp
    sp = lax.axis_index("sp")
    tp = lax.axis_index("tp")
    z = tp // 2
    core = tp % 2
    me = 2 * sp + core
    right = (sp, 2 * ((z + 1) % n_z) + core)
    left = (sp, 2 * ((z + n_z - 1) % n_z) + core)
    partner = (sp, 2 * z + 1 - core)

    def peer_id(index):
        return (index // 2, 2 * z + index % 2)

    def remote(src, dst, send_sem, recv_sem, device):
        return pltpu.make_async_remote_copy(
            src_ref=src,
            dst_ref=dst,
            send_sem=send_sem,
            recv_sem=recv_sem,
            device_id=device,
            device_id_type=MESH,
        )

    own_copies = [
        pltpu.make_async_copy(hbm.at[core], vmem.at[0], own_sem.at[i])
        for i, (hbm, vmem) in enumerate(
            ((gate_hbm, gate_w), (up_hbm, up_w), (down_hbm, down_w))
        )
    ]
    for copy in own_copies:
        copy.start()

    barrier = pltpu.get_barrier_semaphore()

    def greet(k, carry):
        pl.semaphore_signal(
            barrier, inc=1, device_id=peer_id((me + k) % peers), device_id_type=MESH
        )
        return carry

    lax.fori_loop(1, peers, greet, 0)
    for device in (left, right):
        pl.semaphore_signal(barrier, inc=1, device_id=device, device_id_type=MESH)
    pl.semaphore_wait(barrier, peers + 1)

    def hand_copy(k):
        g = (me + k) % peers
        return remote(
            outgoing.at[pl.ds(pl.multiple_of(SLOT * g, SLOT), SLOT)],
            arrived.at[core, pl.ds(pl.multiple_of(SLOT * sp, SLOT), SLOT)],
            hand_send.at[k],
            hand_recv.at[k],
            peer_id(g),
        )

    def hand_start(k, carry):
        hand_copy(k).start()
        return carry

    lax.fori_loop(1, peers, hand_start, 0)
    own_hand = pltpu.make_async_copy(
        outgoing.at[pl.ds(pl.multiple_of(SLOT * me, SLOT), SLOT)],
        arrived.at[core, pl.ds(pl.multiple_of(SLOT * sp, SLOT), SLOT)],
        hand_recv.at[0],
    )
    own_hand.start()

    pair_copies = [
        remote(hbm.at[1 - core], vmem.at[1], pair_send.at[i], pair_recv.at[i], partner)
        for i, (hbm, vmem) in enumerate(
            ((gate_hbm, gate_w), (up_hbm, up_w), (down_hbm, down_w))
        )
    ]
    for copy in pair_copies:
        copy.start()

    own_hand.wait()

    def hand_wait(k, carry):
        g = (me + peers - k) % peers
        slot = arrived.at[g % 2, pl.ds(pl.multiple_of(SLOT * (g // 2), SLOT), SLOT)]
        pltpu.make_async_remote_copy(
            src_ref=outgoing.at[pl.ds(0, SLOT)],
            dst_ref=slot,
            send_sem=hand_send.at[k],
            recv_sem=hand_recv.at[k],
            device_id=peer_id(g),
            device_id_type=MESH,
        ).wait_recv()
        return carry

    lax.fori_loop(1, peers, hand_wait, 0)

    def ring_copy(direction, hop, h):
        block = (z + (n_z - hop + 1 if direction == 0 else hop - 1)) % n_z
        return remote(
            blocks.at[block, h],
            blocks.at[block, h],
            ring_send.at[direction, hop - 1, h],
            ring_recv.at[direction, hop - 1, h],
            right if direction == 0 else left,
        )

    def ring_arrival(direction, hop, h):
        block = (z + (n_z - hop if direction == 0 else hop)) % n_z
        return remote(
            blocks.at[block, h],
            blocks.at[block, h],
            ring_send.at[direction, hop - 1, h],
            ring_recv.at[direction, hop - 1, h],
            right if direction == 0 else left,
        )

    for h in range(2):
        blocks[z, h] = jnp.dot(
            pack[...], arrived[h], preferred_element_type=jnp.float32
        ).astype(jnp.bfloat16)
        for direction in range(2):
            if h == direction or half > 1:
                ring_copy(direction, 1, h).start()

    for copy in own_copies:
        copy.wait()
    for copy in pair_copies:
        copy.wait()

    def sum_send_first(direction):
        block = (z + (half - 1 if direction == 0 else n_z - half + 1)) % n_z
        return remote(
            sums.at[block, direction],
            landing.at[direction, 1, direction],
            sum_send.at[direction, 1, direction],
            sum_recv.at[direction, 1, direction],
            right if direction == 0 else left,
        )

    def expert_step(i, carry):
        hop = (i + 1) // 2

        @pl.when(i % 2 == 1)
        def _():
            for first in range(2):
                for direction in range(2):
                    h = direction if first == 0 else 1 - direction
                    limit = half if h == direction else half - 1

                    @pl.when(hop <= limit)
                    def _(direction=direction, h=h):
                        ring_arrival(direction, hop, h).wait_recv()

                    @pl.when(hop < limit)
                    def _(direction=direction, h=h):
                        ring_copy(direction, hop + 1, h).start()

        block = (z + jnp.where(i % 2 == 1, n_z - hop, hop)) % n_z
        rows = blocks[block].reshape(-1, blocks.shape[-1])
        total = None
        for side in range(2):
            gate_values = jnp.dot(rows, gate_w[side], preferred_element_type=jnp.float32)
            up_values = jnp.dot(rows, up_w[side], preferred_element_type=jnp.float32)
            active = (gate_values / (1.0 + jnp.exp(-gate_values)) * up_values).astype(
                jnp.bfloat16
            )
            part = jnp.dot(active, down_w[side], preferred_element_type=jnp.float32)
            total = part if total is None else total + part
        sums[block] = total.astype(jnp.bfloat16).reshape(sums.shape[1:])

        @pl.when(i == n_z - 2)
        def _():
            for direction in range(2):
                if half > 1:
                    sum_send_first(direction).start()

        return carry

    lax.fori_loop(0, n_z, expert_step, 0)

    def sum_copy(direction, step, h):
        block = (
            z + (half + 1 - step if direction == 0 else n_z - half - 1 + step)
        ) % n_z
        return block, remote(
            sums.at[block, h],
            landing.at[direction, step - 1, h],
            sum_send.at[direction, step - 1, h],
            sum_recv.at[direction, step - 1, h],
            right if direction == 0 else left,
        )

    for direction in range(2):
        sum_copy(direction, 1, 1 - direction)[1].start()
    for step in range(2, half + 1):
        for direction in range(2):
            for h in (1 - direction, direction):
                if h == direction and step == 2:
                    continue
                block, copy = sum_copy(direction, step, h)
                sum_copy(direction, step - 1, h)[1].wait_recv()
                sums[block, h] = (
                    sums[block, h].astype(jnp.float32)
                    + landing[direction, step - 2, h].astype(jnp.float32)
                ).astype(jnp.bfloat16)
                copy.start()

    def back_copy(k):
        g = (me + k) % peers
        return remote(
            sending.at[g % 2, pl.ds(pl.multiple_of(SLOT * (g // 2), SLOT), SLOT)],
            returned.at[pl.ds(pl.multiple_of(SLOT * me, SLOT), SLOT)],
            back_send.at[k],
            back_recv.at[k],
            peer_id(g),
        )

    for h in range(2):
        total = sums[z, h].astype(jnp.float32)
        for direction in range(2):
            if h != direction or half > 1:
                sum_copy(direction, half, h)[1].wait_recv()
                total = total + landing[direction, half - 1, h].astype(jnp.float32)
        sending[h] = jnp.dot(
            spread[...], total.astype(jnp.bfloat16), preferred_element_type=jnp.float32
        ).astype(jnp.bfloat16)

        def back_start(j, carry, h=h):
            k = 2 * j + (h + core) % 2

            @pl.when(k > 0)
            def _():
                back_copy(k).start()

            return carry

        lax.fori_loop(0, n_sp, back_start, 0)

    own_back = pltpu.make_async_copy(
        sending.at[core, pl.ds(pl.multiple_of(SLOT * sp, SLOT), SLOT)],
        returned.at[pl.ds(pl.multiple_of(SLOT * me, SLOT), SLOT)],
        back_recv.at[0],
    )
    own_back.start()

    for direction in range(2):
        for hop in range(1, half + 1):
            for h in range(2):
                if hop <= (half if h == direction else half - 1):
                    ring_copy(direction, hop, h).wait_send()
                if hop > 1 or h != direction:
                    sum_copy(direction, hop, h)[1].wait_send()

    def hand_done(k, carry):
        hand_copy(k).wait_send()
        return carry

    lax.fori_loop(1, peers, hand_done, 0)
    own_back.wait()

    def back_wait(k, carry):
        g = (me + peers - k) % peers
        pltpu.make_async_remote_copy(
            src_ref=sending.at[0, pl.ds(0, SLOT)],
            dst_ref=returned.at[pl.ds(pl.multiple_of(SLOT * g, SLOT), SLOT)],
            send_sem=back_send.at[k],
            recv_sem=back_recv.at[k],
            device_id=peer_id(g),
            device_id_type=MESH,
        ).wait_recv()
        return carry

    lax.fori_loop(1, peers, back_wait, 0)

    def back_done(k, carry):
        back_copy(k).wait_send()
        return carry

    lax.fori_loop(1, peers, back_done, 0)

    weights = mixing[...]
    high = weights.astype(jnp.bfloat16)
    low = (weights - high.astype(jnp.float32)).astype(jnp.bfloat16)
    values = returned[...]
    routed[...] = jnp.dot(high, values, preferred_element_type=jnp.float32) + jnp.dot(
        low, values, preferred_element_type=jnp.float32
    )


def moe(outgoing, mixing, expert_gate, expert_up, expert_down, n_sp, n_z):
    width = outgoing.shape[1]
    hidden_units = expert_gate.shape[2]
    half_rows = n_sp * CAPACITY
    half = n_z // 2
    row = np.arange(half_rows)
    pack = np.zeros((half_rows, n_sp * SLOT), np.float32)
    pack[row, SLOT * (row // CAPACITY) + row % CAPACITY] = 1.0
    vmem = pl.BlockSpec(memory_space=pltpu.VMEM)
    hbm = pl.BlockSpec(memory_space=pl.ANY)
    dma = pltpu.SemaphoreType.DMA
    bf16 = jnp.bfloat16
    return pl.pallas_call(
        functools.partial(moe_kernel, n_sp, n_z),
        out_shape=jax.ShapeDtypeStruct((mixing.shape[0], width), jnp.float32),
        in_specs=[vmem] * 4 + [hbm] * 3,
        out_specs=vmem,
        scratch_shapes=[
            pltpu.VMEM((2, n_sp * SLOT, width), bf16),
            pltpu.VMEM((n_z, 2, half_rows, width), bf16),
            pltpu.VMEM((n_z, 2, half_rows, width), bf16),
            pltpu.VMEM((2, half, 2, half_rows, width), bf16),
            pltpu.VMEM((2, n_sp * SLOT, width), bf16),
            pltpu.VMEM((2 * n_sp * SLOT, width), bf16),
            pltpu.VMEM((2, width, hidden_units), bf16),
            pltpu.VMEM((2, width, hidden_units), bf16),
            pltpu.VMEM((2, hidden_units, width), bf16),
            dma((2 * n_sp,)),
            dma((2 * n_sp,)),
            dma((2, half, 2)),
            dma((2, half, 2)),
            dma((2, half, 2)),
            dma((2, half, 2)),
            dma((2 * n_sp,)),
            dma((2 * n_sp,)),
            dma((3,)),
            dma((3,)),
            dma((3,)),
        ],
        compiler_params=pltpu.CompilerParams(
            collective_id=0, has_side_effects=True, vmem_limit_bytes=56 * 2**20
        ),
        cost_estimate=pl.CostEstimate(
            flops=6_000_000_000, bytes_accessed=10_000_000, transcendentals=1_000_000
        ),
    )(
        outgoing,
        mixing,
        jnp.asarray(pack, bf16),
        jnp.asarray(pack.T, bf16),
        expert_gate,
        expert_up,
        expert_down,
    )


def solution(mesh):
    in_specs = (
        P(("sp", "tp"), None),
        P("sp", "tp"),
        P("sp", "tp"),
        P("sp", None),
        P("sp", None),
        P("sp", None),
        P("sp", None),
        P(),
        P(),
        P(),
        P(),
        P("tp", None),
        P("tp", None),
        P(),
        P(),
        P(("sp", "tp"), None),
        P(("sp", "tp"), None),
        P("sp", None, "tp"),
        P("sp", None, "tp"),
        P("sp", "tp", None),
        P(),
        P(),
        P(),
        P(),
        P(),
    )
    out_specs = P(("sp", "tp"), None)
    return jax.shard_map(local, mesh=mesh, in_specs=in_specs, out_specs=out_specs, check_vma=False)
```

```python
import functools

import jax
import jax.numpy as jnp
import numpy as np
from jax import lax
from jax.experimental import pallas as pl
from jax.experimental.pallas import tpu as pltpu
from jax.sharding import PartitionSpec as P

WIDE_GROUPS = 4
NARROW_GROUPS = 8
GRID_WIDTH = 64
SEQ_SHARDS = 4
LOCAL_EXPERTS = 2


EPS_HEAD = 1e-06
EPS_LAYER = 1e-05
ALPHA = 2.0**0.25
THETA = 10000.0


def layer_norm(values, gain_vec, bias_vec):
    center = jnp.mean(values, axis=-1, keepdims=True)
    shifted = values - center
    variance = jnp.mean(shifted * shifted, axis=-1, keepdims=True)
    return (shifted * lax.rsqrt(variance + EPS_LAYER) * gain_vec + bias_vec).astype(jnp.bfloat16)


def local(
    residual,
    wide_query,
    narrow_query,
    wide_keys,
    narrow_keys,
    wide_values,
    narrow_values,
    wide_query_gain,
    wide_key_gain,
    narrow_query_gain,
    narrow_key_gain,
    wide_out,
    narrow_out,
    first_gain,
    first_bias,
    route_ids,
    route_weights,
    expert_gate,
    expert_up,
    expert_down,
    shared_gate,
    shared_up,
    shared_down,
    second_gain,
    second_bias,
):
    projected = attention(
        wide_query,
        narrow_query,
        wide_keys,
        narrow_keys,
        wide_values,
        narrow_values,
        wide_query_gain,
        wide_key_gain,
        narrow_query_gain,
        narrow_key_gain,
        wide_out,
        narrow_out,
        lax.axis_size("tp") // 2,
    )
    hidden = layer_norm(ALPHA * residual.astype(jnp.float32) + projected, first_gain, first_bias)
    device_rows = hidden.shape[0]
    sp_size = lax.axis_size("sp")
    top_count = route_ids.shape[1]
    experts = LOCAL_EXPERTS * sp_size
    flat_ids = route_ids.reshape(-1)
    expert_hits = (flat_ids[:, None] == jnp.arange(experts, dtype=jnp.int32)[None, :]).astype(
        jnp.int32
    )
    earlier = jnp.sum((jnp.cumsum(expert_hits, axis=0) - expert_hits) * expert_hits, axis=1)
    slot_index = flat_ids * SLOT + earlier
    chosen = (
        slot_index[:, None] == jnp.arange(experts * SLOT, dtype=jnp.int32)[None, :]
    ).astype(jnp.float32)
    chosen = chosen.reshape(device_rows, top_count, experts * SLOT)
    placing = jnp.sum(chosen, axis=1).astype(jnp.bfloat16)
    mixing = jnp.sum(chosen * route_weights[:, :, None], axis=1)
    outgoing = jnp.einsum("rs,rd->sd", placing, hidden, preferred_element_type=jnp.float32).astype(
        jnp.bfloat16
    )
    routed = moe(
        outgoing,
        mixing,
        expert_gate,
        expert_up,
        expert_down,
        sp_size,
        lax.axis_size("tp") // 2,
    )
    shared_gate_values = jnp.dot(hidden, shared_gate, preferred_element_type=jnp.float32)
    shared_up_values = jnp.dot(hidden, shared_up, preferred_element_type=jnp.float32)
    shared_active = (jax.nn.silu(shared_gate_values) * shared_up_values).astype(jnp.bfloat16)
    shared_output = jnp.dot(shared_active, shared_down, preferred_element_type=jnp.float32)
    return layer_norm(
        ALPHA * hidden.astype(jnp.float32) + routed + shared_output, second_gain, second_bias
    )


CAPACITY = 5
SLOT = 8
MESH = pl.DeviceIdType.MESH


def dot_rows(a, b):
    return lax.dot_general(
        a, b, (((1,), (1,)), ((), ())), preferred_element_type=jnp.float32
    )


def moe_kernel(
    n_sp,
    n_z,
    outgoing,
    mixing,
    pack,
    spread,
    gate_hbm,
    up_hbm,
    down_hbm,
    routed,
    arrived,
    blocks,
    sums,
    landing,
    sending,
    returned,
    gate_w,
    up_w,
    down_w,
    hand_send,
    hand_recv,
    ring_send,
    ring_recv,
    sum_send,
    sum_recv,
    back_send,
    back_recv,
    own_sem,
    pair_send,
    pair_recv,
):
    half = n_z // 2
    peers = 2 * n_sp
    sp = lax.axis_index("sp")
    tp = lax.axis_index("tp")
    z = tp // 2
    core = tp % 2
    me = 2 * sp + core
    right = (sp, 2 * ((z + 1) % n_z) + core)
    left = (sp, 2 * ((z + n_z - 1) % n_z) + core)
    partner = (sp, 2 * z + 1 - core)

    def peer_id(index):
        return (index // 2, 2 * z + index % 2)

    def remote(src, dst, send_sem, recv_sem, device):
        return pltpu.make_async_remote_copy(
            src_ref=src,
            dst_ref=dst,
            send_sem=send_sem,
            recv_sem=recv_sem,
            device_id=device,
            device_id_type=MESH,
        )

    own_copies = [
        pltpu.make_async_copy(hbm.at[core], vmem.at[0], own_sem.at[i])
        for i, (hbm, vmem) in enumerate(
            ((gate_hbm, gate_w), (up_hbm, up_w), (down_hbm, down_w))
        )
    ]
    for copy in own_copies:
        copy.start()

    barrier = pltpu.get_barrier_semaphore()

    def greet(k, carry):
        pl.semaphore_signal(
            barrier, inc=1, device_id=peer_id((me + k) % peers), device_id_type=MESH
        )
        return carry

    lax.fori_loop(1, peers, greet, 0)
    for device in (left, right):
        pl.semaphore_signal(barrier, inc=1, device_id=device, device_id_type=MESH)
    pl.semaphore_wait(barrier, peers + 1)

    def hand_copy(k):
        g = (me + k) % peers
        return remote(
            outgoing.at[pl.ds(pl.multiple_of(SLOT * g, SLOT), SLOT)],
            arrived.at[core, pl.ds(pl.multiple_of(SLOT * sp, SLOT), SLOT)],
            hand_send.at[k],
            hand_recv.at[k],
            peer_id(g),
        )

    def hand_start(k, carry):
        hand_copy(k).start()
        return carry

    lax.fori_loop(1, peers, hand_start, 0)
    own_hand = pltpu.make_async_copy(
        outgoing.at[pl.ds(pl.multiple_of(SLOT * me, SLOT), SLOT)],
        arrived.at[core, pl.ds(pl.multiple_of(SLOT * sp, SLOT), SLOT)],
        hand_recv.at[0],
    )
    own_hand.start()

    pair_copies = [
        remote(hbm.at[1 - core], vmem.at[1], pair_send.at[i], pair_recv.at[i], partner)
        for i, (hbm, vmem) in enumerate(
            ((gate_hbm, gate_w), (up_hbm, up_w), (down_hbm, down_w))
        )
    ]
    for copy in pair_copies:
        copy.start()

    own_hand.wait()

    def hand_wait(k, carry):
        g = (me + peers - k) % peers
        slot = arrived.at[g % 2, pl.ds(pl.multiple_of(SLOT * (g // 2), SLOT), SLOT)]
        pltpu.make_async_remote_copy(
            src_ref=outgoing.at[pl.ds(0, SLOT)],
            dst_ref=slot,
            send_sem=hand_send.at[k],
            recv_sem=hand_recv.at[k],
            device_id=peer_id(g),
            device_id_type=MESH,
        ).wait_recv()
        return carry

    lax.fori_loop(1, peers, hand_wait, 0)

    def ring_copy(direction, hop, h):
        block = (z + (n_z - hop + 1 if direction == 0 else hop - 1)) % n_z
        return remote(
            blocks.at[block, h],
            blocks.at[block, h],
            ring_send.at[direction, hop - 1, h],
            ring_recv.at[direction, hop - 1, h],
            right if direction == 0 else left,
        )

    def ring_arrival(direction, hop, h):
        block = (z + (n_z - hop if direction == 0 else hop)) % n_z
        return remote(
            blocks.at[block, h],
            blocks.at[block, h],
            ring_send.at[direction, hop - 1, h],
            ring_recv.at[direction, hop - 1, h],
            right if direction == 0 else left,
        )

    for h in range(2):
        blocks[z, h] = jnp.dot(
            pack[...], arrived[h], preferred_element_type=jnp.float32
        ).astype(jnp.bfloat16)
        for direction in range(2):
            if h == direction or half > 1:
                ring_copy(direction, 1, h).start()

    for copy in own_copies:
        copy.wait()
    for copy in pair_copies:
        copy.wait()

    def sum_send_first(direction):
        block = (z + (half - 1 if direction == 0 else n_z - half + 1)) % n_z
        return remote(
            sums.at[block, direction],
            landing.at[direction, 1, direction],
            sum_send.at[direction, 1, direction],
            sum_recv.at[direction, 1, direction],
            right if direction == 0 else left,
        )

    def expert_step(i, carry):
        hop = (i + 1) // 2

        @pl.when(i % 2 == 1)
        def _():
            for first in range(2):
                for direction in range(2):
                    h = direction if first == 0 else 1 - direction
                    limit = half if h == direction else half - 1

                    @pl.when(hop <= limit)
                    def _(direction=direction, h=h):
                        ring_arrival(direction, hop, h).wait_recv()

                    @pl.when(hop < limit)
                    def _(direction=direction, h=h):
                        ring_copy(direction, hop + 1, h).start()

        block = (z + jnp.where(i % 2 == 1, n_z - hop, hop)) % n_z
        rows = blocks[block].reshape(-1, blocks.shape[-1])
        total = None
        for side in range(2):
            gate_values = dot_rows(rows, gate_w[side])
            up_values = dot_rows(rows, up_w[side])
            active = (gate_values / (1.0 + jnp.exp(-gate_values)) * up_values).astype(
                jnp.bfloat16
            )
            part = jnp.dot(active, down_w[side], preferred_element_type=jnp.float32)
            total = part if total is None else total + part
        sums[block] = total.astype(jnp.bfloat16).reshape(sums.shape[1:])

        @pl.when(i == n_z - 2)
        def _():
            for direction in range(2):
                if half > 1:
                    sum_send_first(direction).start()

        return carry

    lax.fori_loop(0, n_z, expert_step, 0)

    def sum_copy(direction, step, h):
        block = (
            z + (half + 1 - step if direction == 0 else n_z - half - 1 + step)
        ) % n_z
        return block, remote(
            sums.at[block, h],
            landing.at[direction, step - 1, h],
            sum_send.at[direction, step - 1, h],
            sum_recv.at[direction, step - 1, h],
            right if direction == 0 else left,
        )

    for direction in range(2):
        sum_copy(direction, 1, 1 - direction)[1].start()
    for step in range(2, half + 1):
        for direction in range(2):
            for h in (1 - direction, direction):
                if h == direction and step == 2:
                    continue
                block, copy = sum_copy(direction, step, h)
                sum_copy(direction, step - 1, h)[1].wait_recv()
                sums[block, h] = (
                    sums[block, h].astype(jnp.float32)
                    + landing[direction, step - 2, h].astype(jnp.float32)
                ).astype(jnp.bfloat16)
                copy.start()

    def back_copy(k):
        g = (me + k) % peers
        return remote(
            sending.at[g % 2, pl.ds(pl.multiple_of(SLOT * (g // 2), SLOT), SLOT)],
            returned.at[pl.ds(pl.multiple_of(SLOT * me, SLOT), SLOT)],
            back_send.at[k],
            back_recv.at[k],
            peer_id(g),
        )

    for h in range(2):
        total = sums[z, h].astype(jnp.float32)
        for direction in range(2):
            if h != direction or half > 1:
                sum_copy(direction, half, h)[1].wait_recv()
                total = total + landing[direction, half - 1, h].astype(jnp.float32)
        sending[h] = jnp.dot(
            spread[...], total.astype(jnp.bfloat16), preferred_element_type=jnp.float32
        ).astype(jnp.bfloat16)

        def back_start(j, carry, h=h):
            k = 2 * j + (h + core) % 2

            @pl.when(k > 0)
            def _():
                back_copy(k).start()

            return carry

        lax.fori_loop(0, n_sp, back_start, 0)

    own_back = pltpu.make_async_copy(
        sending.at[core, pl.ds(pl.multiple_of(SLOT * sp, SLOT), SLOT)],
        returned.at[pl.ds(pl.multiple_of(SLOT * me, SLOT), SLOT)],
        back_recv.at[0],
    )
    own_back.start()

    for direction in range(2):
        for hop in range(1, half + 1):
            for h in range(2):
                if hop <= (half if h == direction else half - 1):
                    ring_copy(direction, hop, h).wait_send()
                if hop > 1 or h != direction:
                    sum_copy(direction, hop, h)[1].wait_send()

    def hand_done(k, carry):
        hand_copy(k).wait_send()
        return carry

    lax.fori_loop(1, peers, hand_done, 0)
    own_back.wait()

    def back_wait(k, carry):
        g = (me + peers - k) % peers
        pltpu.make_async_remote_copy(
            src_ref=sending.at[0, pl.ds(0, SLOT)],
            dst_ref=returned.at[pl.ds(pl.multiple_of(SLOT * g, SLOT), SLOT)],
            send_sem=back_send.at[k],
            recv_sem=back_recv.at[k],
            device_id=peer_id(g),
            device_id_type=MESH,
        ).wait_recv()
        return carry

    lax.fori_loop(1, peers, back_wait, 0)

    def back_done(k, carry):
        back_copy(k).wait_send()
        return carry

    lax.fori_loop(1, peers, back_done, 0)

    weights = mixing[...]
    high = weights.astype(jnp.bfloat16)
    low = (weights - high.astype(jnp.float32)).astype(jnp.bfloat16)
    values = returned[...]
    routed[...] = jnp.dot(high, values, preferred_element_type=jnp.float32) + jnp.dot(
        low, values, preferred_element_type=jnp.float32
    )


def moe(outgoing, mixing, expert_gate, expert_up, expert_down, n_sp, n_z):
    width = outgoing.shape[1]
    hidden_units = expert_gate.shape[2]
    half_rows = n_sp * CAPACITY
    half = n_z // 2
    row = np.arange(half_rows)
    pack = np.zeros((half_rows, n_sp * SLOT), np.float32)
    pack[row, SLOT * (row // CAPACITY) + row % CAPACITY] = 1.0
    vmem = pl.BlockSpec(memory_space=pltpu.VMEM)
    hbm = pl.BlockSpec(memory_space=pl.ANY)
    dma = pltpu.SemaphoreType.DMA
    bf16 = jnp.bfloat16
    return pl.pallas_call(
        functools.partial(moe_kernel, n_sp, n_z),
        out_shape=jax.ShapeDtypeStruct((mixing.shape[0], width), jnp.float32),
        in_specs=[vmem] * 4 + [hbm] * 3,
        out_specs=vmem,
        scratch_shapes=[
            pltpu.VMEM((2, n_sp * SLOT, width), bf16),
            pltpu.VMEM((n_z, 2, half_rows, width), bf16),
            pltpu.VMEM((n_z, 2, half_rows, width), bf16),
            pltpu.VMEM((2, half, 2, half_rows, width), bf16),
            pltpu.VMEM((2, n_sp * SLOT, width), bf16),
            pltpu.VMEM((2 * n_sp * SLOT, width), bf16),
            pltpu.VMEM((2, hidden_units, width), bf16),
            pltpu.VMEM((2, hidden_units, width), bf16),
            pltpu.VMEM((2, hidden_units, width), bf16),
            dma((2 * n_sp,)),
            dma((2 * n_sp,)),
            dma((2, half, 2)),
            dma((2, half, 2)),
            dma((2, half, 2)),
            dma((2, half, 2)),
            dma((2 * n_sp,)),
            dma((2 * n_sp,)),
            dma((3,)),
            dma((3,)),
            dma((3,)),
        ],
        compiler_params=pltpu.CompilerParams(
            collective_id=0, has_side_effects=True, vmem_limit_bytes=56 * 2**20
        ),
        cost_estimate=pl.CostEstimate(
            flops=6_000_000_000, bytes_accessed=10_000_000, transcendentals=1_000_000
        ),
    )(
        outgoing,
        mixing,
        jnp.asarray(pack, bf16),
        jnp.asarray(pack.T, bf16),
        jnp.swapaxes(expert_gate, 1, 2),
        jnp.swapaxes(expert_up, 1, 2),
        expert_down,
    )


LANES = 256
LOG2E = 1.4426950408889634


def iota2(shape, axis):
    return lax.broadcasted_iota(jnp.int32, shape, axis)


def selection(rows, column_of_lane, offset, first, last):
    lane = iota2((rows, LANES), 1)
    row = iota2((rows, LANES), 0)
    inside = jnp.logical_and(lane >= first, lane < last)
    hit = jnp.logical_and(inside, row == column_of_lane(lane - first) + offset)
    return jnp.where(hit, 1.0, 0.0).astype(jnp.bfloat16)


def flip(apart):
    return lambda lane: lane + apart - 2 * apart * ((lane // apart) % 2)


def same(lane):
    return lane


def bf16_dot(a, b):
    return jnp.dot(a, b, preferred_element_type=jnp.float32)


def turned_dot(a, b):
    return lax.dot_general(
        a, b, (((0,), (0,)), ((), ())), preferred_element_type=jnp.float32
    )


def turned(raw, swapped_raw, mean_matrix, row_tables, tables, gains, first_row, rows):
    square = raw * raw
    high = square.astype(jnp.bfloat16)
    low = (square - high.astype(jnp.float32)).astype(jnp.bfloat16)
    mean_square = bf16_dot(high, mean_matrix) + bf16_dot(low, mean_matrix)
    shape = (rows * GRID_WIDTH, LANES)
    cosine = (row_tables[0, pl.ds(first_row, rows)] + tables[0][None]).reshape(shape)
    sine = (row_tables[1, pl.ds(first_row, rows)] + tables[1][None]).reshape(shape)
    mixed = raw * (cosine * gains[0:1]) + swapped_raw * (sine * gains[1:2])
    return mixed * lax.rsqrt(mean_square + EPS_HEAD)


def attention_kernel(
    n_z,
    wide_query,
    narrow_query,
    wide_keys,
    narrow_keys,
    wide_values,
    narrow_values,
    gains,
    row_tables,
    tables,
    out_rows,
    projected,
    own_kv,
    kv,
    queries,
    totals,
    largest,
    mixed,
    mixed_in,
    sums,
    landing,
    weights,
    final_out,
    final_in,
    kv_send,
    kv_recv,
    far_send,
    far_recv,
    pass_send,
    pass_recv,
    mixed_send,
    mixed_recv,
    sum_send,
    sum_recv,
    weight_sem,
    weight_send,
    weight_recv,
    final_send,
    final_recv,
):
    half = n_z // 2
    sp = lax.axis_index("sp")
    tp = lax.axis_index("tp")
    z = tp // 2
    core = tp % 2
    x = sp % SEQ_SHARDS
    row_start = sp - x
    right = (sp, 2 * ((z + 1) % n_z) + core)
    left = (sp, 2 * ((z + n_z - 1) % n_z) + core)
    east = (row_start + (x + 1) % SEQ_SHARDS, tp)
    west = (row_start + (x + SEQ_SHARDS - 1) % SEQ_SHARDS, tp)
    partner = (sp, 2 * z + 1 - core)
    quarter = kv.shape[2]
    columns = weights.shape[2]
    chip_rows = queries.shape[2]
    core_rows = chip_rows // 2

    def remote(src, dst, send_sem, recv_sem, device):
        return pltpu.make_async_remote_copy(
            src_ref=src,
            dst_ref=dst,
            send_sem=send_sem,
            recv_sem=recv_sem,
            device_id=device,
            device_id_type=MESH,
        )

    def column_half(which):
        return out_rows.at[:, pl.ds(pl.multiple_of(which * columns, columns), columns)]

    own_weights = pltpu.make_async_copy(column_half(core), weights.at[0], weight_sem)
    own_weights.start()
    barrier = pltpu.get_barrier_semaphore()
    for device in (right, left, east, west, partner):
        pl.semaphore_signal(barrier, inc=1, device_id=device, device_id_type=MESH)

    wide_group = tp * WIDE_GROUPS // (2 * n_z)
    narrow_group = tp * NARROW_GROUPS // (2 * n_z)
    lane_in = iota2((LANES, LANES), 0)
    lane_out = iota2((LANES, LANES), 1)
    both_wide = jnp.logical_and(lane_in < 64, lane_out < 64)
    both_narrow = jnp.logical_and(
        jnp.logical_and(lane_in >= 128, lane_in < 160),
        jnp.logical_and(lane_out >= 128, lane_out < 160),
    )
    mean_matrix = jnp.where(both_wide, 1.0 / 64, jnp.where(both_narrow, 1.0 / 32, 0.0)).astype(
        jnp.bfloat16
    )
    key_in = wide_keys.shape[1]
    wide_same = selection(key_in, same, 64 * wide_group, 0, 64)
    wide_flip = selection(key_in, flip(16), 64 * wide_group, 0, 64)
    narrow_same = selection(key_in, same, 32 * narrow_group, 128, 160)
    narrow_flip = selection(key_in, flip(8), 32 * narrow_group, 128, 160)
    wide_place = selection(key_in, same, 64 * wide_group, 64, 128)
    narrow_place = selection(key_in, same, 32 * narrow_group, 160, 192) + selection(
        key_in, same, 32 * narrow_group, 224, 256
    )
    lane = iota2((1, LANES), 1)
    ones = jnp.where(jnp.logical_and(lane >= 192, lane < 224), 1.0, 0.0)
    grid_rows = quarter // GRID_WIDTH
    first_row = x * (SEQ_SHARDS * grid_rows)

    def kv_copy(to_east):
        return remote(
            own_kv.at[pl.ds(2 * core, 2)],
            kv.at[x, pl.ds(2 * core, 2)],
            kv_send.at[to_east],
            kv_recv.at[to_east],
            west if to_east == 0 else east,
        )

    def kv_arrival(to_east):
        source = (x + (SEQ_SHARDS - 1 if to_east == 1 else 1)) % SEQ_SHARDS
        return source, remote(
            own_kv.at[pl.ds(2 * core, 2)],
            kv.at[source, pl.ds(2 * core, 2)],
            kv_send.at[to_east],
            kv_recv.at[to_east],
            west if to_east == 0 else east,
        )

    def far_copy(to_east, arriving):
        source = (x + (SEQ_SHARDS - 1 if to_east == 1 else 1)) % SEQ_SHARDS
        block = (x + 2) % SEQ_SHARDS if arriving else source
        part = 2 * core + (0 if to_east == 1 else 1)
        return remote(
            kv.at[block, part],
            kv.at[block, part],
            far_send.at[to_east],
            far_recv.at[to_east],
            west if to_east == 0 else east,
        )

    def pass_copy(to_east, side):
        source = (x + (SEQ_SHARDS - 1 if to_east == 1 else 1)) % SEQ_SHARDS
        at = pl.ds(2 * side, 2)
        return remote(
            kv.at[source, at],
            kv.at[source, at],
            pass_send.at[to_east],
            pass_recv.at[to_east],
            partner,
        )

    def pass_far(to_east, side):
        block = (x + 2) % SEQ_SHARDS
        part = 2 * side + (0 if to_east == 1 else 1)
        return remote(
            kv.at[block, part],
            kv.at[block, part],
            pass_send.at[2 + to_east],
            pass_recv.at[2 + to_east],
            partner,
        )

    def prepare_keys(i, carry):
        part = (2 * core + i) % 4
        at = pl.ds(pl.multiple_of(part * quarter, quarter), quarter)
        wide = wide_keys[at, :]
        narrow = narrow_keys[at, :]
        raw = bf16_dot(wide, wide_same) + bf16_dot(narrow, narrow_same)
        other = bf16_dot(wide, wide_flip) + bf16_dot(narrow, narrow_flip)
        keys = turned(
            raw,
            other,
            mean_matrix,
            row_tables,
            tables,
            gains[0:2],
            first_row + part * grid_rows,
            grid_rows,
        )
        values = bf16_dot(wide_values[at, :], wide_place) + bf16_dot(
            narrow_values[at, :], narrow_place
        )
        own_kv[part] = (keys + values + ones).astype(jnp.bfloat16)
        return carry

    lax.fori_loop(0, 2, prepare_keys, 0)
    pl.semaphore_wait(barrier, 5)
    for to_east in range(2):
        kv_copy(to_east).start()
    partner_weights = remote(
        column_half(1 - core), weights.at[1], weight_send, weight_recv, partner
    )
    partner_weights.start()
    lax.fori_loop(2, 4, prepare_keys, 0)

    scales = (64**-0.5 * LOG2E, 32**-0.5 * LOG2E, 32**-0.5 * LOG2E)

    def attend(chunk, keys, start):
        for head in range(3):
            scores = lax.dot_general(
                queries[chunk, head],
                keys,
                (((1,), (1,)), ((), ())),
                preferred_element_type=jnp.float32,
            )
            peak = jnp.max(scores, axis=-1, keepdims=True)
            if not start:
                before = largest[chunk, head][:, 0:1]
                peak = jnp.maximum(before, peak)
            parts = jnp.exp2((scores - peak) * scales[head]).astype(jnp.bfloat16)
            fresh = bf16_dot(parts, keys)
            if not start:
                fresh = fresh + totals[chunk, head] * jnp.exp2((before - peak) * scales[head])
            totals[chunk, head] = fresh
            largest[chunk, head] = jnp.broadcast_to(peak, (chip_rows, 128))

    def chunk_of(i):
        hop = half - (i + 1) // 2
        return (z + jnp.where(i % 2 == 1, hop, n_z - hop)) % n_z

    query_in = wide_query.shape[0]
    query_same = (
        selection(query_in, same, 0, 0, 64),
        selection(query_in, same, 0, 128, 160),
        selection(query_in, same, 32, 128, 160),
    )
    query_flip = (
        selection(query_in, flip(16), 0, 0, 64),
        selection(query_in, flip(8), 0, 128, 160),
        selection(query_in, flip(8), 32, 128, 160),
    )

    def own_step(i, carry):
        chunk = chunk_of(i)
        at = pl.ds(pl.multiple_of(chunk * chip_rows, chip_rows), chip_rows)
        chunk_grid = chip_rows // GRID_WIDTH
        for head in range(3):
            rows = (wide_query if head == 0 else narrow_query)[:, at]
            queries[chunk, head] = turned(
                turned_dot(rows, query_same[head]),
                turned_dot(rows, query_flip[head]),
                mean_matrix,
                row_tables,
                tables,
                gains[2:4],
                first_row + chunk * chunk_grid,
                chunk_grid,
            ).astype(jnp.bfloat16)
        attend(chunk, own_kv[...].reshape(-1, LANES), True)
        return carry

    lax.fori_loop(0, n_z, own_step, 0)

    for to_east in range(2):
        kv_arrival(to_east)[1].wait_recv()
        far_copy(to_east, False).start()
        pass_copy(to_east, core).start()
    for to_east in range(2):
        pass_copy(to_east, 1 - core).wait_recv()

    def next_block(i, b, carry):
        block = (x + 3 - 2 * b + 3 * (b * (b - 1) // 2)) % SEQ_SHARDS
        attend(chunk_of(i), kv[block].reshape(-1, LANES), False)
        return carry

    def near_step(j, carry):
        return next_block(half + j // 2, j % 2, carry)

    lax.fori_loop(0, 2 * (n_z - half), near_step, 0)

    for to_east in range(2):
        far_copy(to_east, True).wait_recv()
        pass_far(to_east, core).start()
    for to_east in range(2):
        pass_far(to_east, 1 - core).wait_recv()
    own_weights.wait()
    partner_weights.wait()

    def mixed_copy(i):
        return remote(
            mixed.at[i], mixed_in.at[i], mixed_send.at[i], mixed_recv.at[i], partner
        )

    def sum_copy(direction, step, h):
        block = (
            z + (half + 1 - step if direction == 0 else n_z - half - 1 + step)
        ) % n_z
        return block, remote(
            sums.at[block, h],
            landing.at[direction, step - 1, h],
            sum_send.at[direction, step - 1, h],
            sum_recv.at[direction, step - 1, h],
            right if direction == 0 else left,
        )

    def add_and_send(direction, step, h):
        block, copy = sum_copy(direction, step, h)
        sum_copy(direction, step - 1, h)[1].wait_recv()
        sums[block, h] = (
            sums[block, h].astype(jnp.float32) + landing[direction, step - 2, h].astype(jnp.float32)
        ).astype(jnp.bfloat16)
        copy.start()

    def step_body(i, carry):
        @pl.when(i < n_z)
        def _():
            lax.fori_loop(
                jnp.where(i < half, 0, 2), 3, functools.partial(next_block, i), 0
            )
            chunk = chunk_of(i)
            joined = None
            for head, (first, last) in enumerate(((64, 128), (160, 192), (224, 256))):
                part = totals[chunk, head]
                part = part / part[:, 192:193]
                inside = jnp.logical_and(lane >= first, lane < last)
                part = jnp.where(inside, part, 0.0)
                joined = part if joined is None else joined + part
            mixed[i] = joined.astype(jnp.bfloat16)
            mixed_copy(i).start()

        @pl.when(i >= 1)
        def _():
            j = i - 1
            chunk = chunk_of(j)
            mixed_copy(j).wait_recv()
            total = bf16_dot(mixed[j], weights[0]) + bf16_dot(mixed_in[j], weights[1])
            sums[chunk] = total.astype(jnp.bfloat16).reshape(sums.shape[1:])

            @pl.when(j == 0)
            def _():
                for direction in range(2):
                    sum_copy(direction, 1, 1 - direction)[1].start()

            if half > 1:

                @pl.when(j == 1)
                def _():
                    sum_copy(0, 2, 0)[1].start()

                @pl.when(j == 2)
                def _():
                    sum_copy(1, 2, 1)[1].start()

        @pl.when(jnp.logical_and(i >= 3, i <= n_z))
        def _():
            step = (i - 1) // 2 + 1
            for direction in range(2):

                @pl.when((i - 1) % 2 == direction)
                def _(direction=direction):
                    add_and_send(direction, step, 1 - direction)

                    @pl.when(step > 2)
                    def _():
                        add_and_send(direction, step, direction)

        return carry

    lax.fori_loop(0, n_z + 1, step_body, 0)

    for h in range(2):
        total = sums[z, h].astype(jnp.float32)
        for direction in range(2):
            if h != direction or half > 1:
                sum_copy(direction, half, h)[1].wait_recv()
                total = total + landing[direction, half - 1, h].astype(jnp.float32)
        final_out[h] = total

    final_copy = remote(final_out.at[1 - core], final_in, final_send, final_recv, partner)
    final_copy.start()

    for to_east in range(2):
        kv_copy(to_east).wait_send()
        far_copy(to_east, False).wait_send()
        pass_copy(to_east, core).wait_send()
        pass_far(to_east, core).wait_send()
    for direction in range(2):
        for hop in range(1, half + 1):
            for h in range(2):
                if hop > 1 or h != direction:
                    sum_copy(direction, hop, h)[1].wait_send()

    def mixed_done(i, carry):
        mixed_copy(i).wait_send()
        return carry

    lax.fori_loop(0, n_z, mixed_done, 0)
    final_copy.wait()
    for which in range(2):

        @pl.when(core == which)
        def _(which=which):
            projected[:, which * columns : (which + 1) * columns] = final_out[which]
            projected[:, (1 - which) * columns : (2 - which) * columns] = final_in[...]


def turn_tables():
    tables = np.zeros((4, GRID_WIDTH, LANES), np.float64)
    for first, size in ((0, 64), (128, 32)):
        n = size // 4
        angle = np.arange(GRID_WIDTH)[:, None] * THETA ** (-np.arange(n)[None, :] / n)
        cosine = np.concatenate([np.cos(angle)] * 2, axis=1)
        sine = np.concatenate([-np.sin(angle), np.sin(angle)], axis=1)
        tables[0, :, first : first + 2 * n] = cosine
        tables[1, :, first : first + 2 * n] = sine
        tables[2, :, first + 2 * n : first + 4 * n] = cosine
        tables[3, :, first + 2 * n : first + 4 * n] = sine
    tables = tables.astype(np.float32)
    return tables[:2, :, None, :], tables[2:]


def lane_gain(wide_gain, narrow_gain, flipped):
    if flipped:
        wide_gain = wide_gain.reshape(2, 2, 16)[:, ::-1].reshape(-1)
        narrow_gain = narrow_gain.reshape(2, 2, 8)[:, ::-1].reshape(-1)
    zeros = jnp.zeros((64,), jnp.float32)
    return jnp.concatenate([wide_gain, zeros, narrow_gain, zeros, zeros[:32]])


def attention(
    wide_query,
    narrow_query,
    wide_keys,
    narrow_keys,
    wide_values,
    narrow_values,
    wide_query_gain,
    wide_key_gain,
    narrow_query_gain,
    narrow_key_gain,
    wide_out,
    narrow_out,
    n_z,
):
    rows = wide_query.shape[0]
    chip_rows = rows // n_z
    width = wide_out.shape[1]
    half = n_z // 2
    gains = jnp.stack(
        [
            lane_gain(wide_key_gain, narrow_key_gain, False),
            lane_gain(wide_key_gain, narrow_key_gain, True),
            lane_gain(wide_query_gain, narrow_query_gain, False),
            lane_gain(wide_query_gain, narrow_query_gain, True),
        ]
    )
    row_tables, tables = turn_tables()
    gap = jnp.zeros((64, width), jnp.bfloat16)
    out_rows = jnp.concatenate(
        [gap, wide_out, gap[:32], narrow_out[:32], gap[:32], narrow_out[32:]], axis=0
    )
    vmem = pl.BlockSpec(memory_space=pltpu.VMEM)
    dma = pltpu.SemaphoreType.DMA
    bf16 = jnp.bfloat16
    f32 = jnp.float32
    return pl.pallas_call(
        functools.partial(attention_kernel, n_z),
        out_shape=jax.ShapeDtypeStruct((chip_rows // 2, width), f32),
        in_specs=[vmem] * 10,
        out_specs=vmem,
        scratch_shapes=[
            pltpu.VMEM((4, rows // 4, LANES), bf16),
            pltpu.VMEM((SEQ_SHARDS, 4, rows // 4, LANES), bf16),
            pltpu.VMEM((n_z, 3, chip_rows, LANES), bf16),
            pltpu.VMEM((n_z, 3, chip_rows, LANES), f32),
            pltpu.VMEM((n_z, 3, chip_rows, 128), f32),
            pltpu.VMEM((n_z, chip_rows, LANES), bf16),
            pltpu.VMEM((n_z, chip_rows, LANES), bf16),
            pltpu.VMEM((n_z, 2, chip_rows // 2, width // 2), bf16),
            pltpu.VMEM((2, half, 2, chip_rows // 2, width // 2), bf16),
            pltpu.VMEM((2, LANES, width // 2), bf16),
            pltpu.VMEM((2, chip_rows // 2, width // 2), f32),
            pltpu.VMEM((chip_rows // 2, width // 2), f32),
            dma((2,)),
            dma((2,)),
            dma((2,)),
            dma((2,)),
            dma((4,)),
            dma((4,)),
            dma((n_z,)),
            dma((n_z,)),
            dma((2, half, 2)),
            dma((2, half, 2)),
            dma,
            dma,
            dma,
            dma,
            dma,
        ],
        compiler_params=pltpu.CompilerParams(
            collective_id=1, has_side_effects=True, vmem_limit_bytes=56 * 2**20
        ),
        cost_estimate=pl.CostEstimate(
            flops=13_000_000_000, bytes_accessed=6_000_000, transcendentals=13_000_000
        ),
    )(
        wide_query.T,
        narrow_query.T,
        wide_keys,
        narrow_keys,
        wide_values,
        narrow_values,
        gains,
        jnp.asarray(row_tables),
        jnp.asarray(tables),
        out_rows,
    )


def solution(mesh):
    in_specs = (
        P(("sp", "tp"), None),
        P("sp", "tp"),
        P("sp", "tp"),
        P("sp", None),
        P("sp", None),
        P("sp", None),
        P("sp", None),
        P(),
        P(),
        P(),
        P(),
        P("tp", None),
        P("tp", None),
        P(),
        P(),
        P(("sp", "tp"), None),
        P(("sp", "tp"), None),
        P("sp", None, "tp"),
        P("sp", None, "tp"),
        P("sp", "tp", None),
        P(),
        P(),
        P(),
        P(),
        P(),
    )
    out_specs = P(("sp", "tp"), None)
    return jax.shard_map(local, mesh=mesh, in_specs=in_specs, out_specs=out_specs, check_vma=False)
```
